32 devices in a mesh: sp: 16 (over z, y, x), tp: 2 (over core).
Axes of the slice: x: 2, y: 2, z: 4, core: 2. Of those that a mesh axis runs over, the one named last changes fastest.
Arguments:
- tokens_in: bfloat16 [2048, 2048], P(('sp', 'tp')), may hold values from -9 to 9, as said below
- w_query: bfloat16 [2048, 2048], P(None, 'tp'), may hold values from -0.125 to 0.125
- w_key: bfloat16 [2048, 512], P(None, 'tp'), may hold values from -0.125 to 0.125
- w_value: bfloat16 [2048, 512], P(None, 'tp'), may hold values from -0.125 to 0.125
- w_out: bfloat16 [2048, 2048], P('tp'), may hold values from -0.125 to 0.125
- q_gain: float32 [64], replicated, may hold values from 0.1 to 14
- k_gain: float32 [64], replicated, may hold values from 0.1 to 14
Outputs:
- attended: bfloat16 [2048, 2048], P(('sp', 'tp'))
The draws below stay inside these ranges and needn't reach their ends.
Inputs may be any that keep to these rules, and one draw needn't show every extreme that they name: `tokens_in`: activations whose mean differs from one block of 128 tokens to another.
All inputs are finite; a program needn't handle non-finite values.
Results may differ from the reference program's by a relative error of at most 0.014.
The reference program's roundings to bfloat16 on the way (of `weights` and `mixed`) count: a program that leaves them out, or rounds other values in their place, can miss the bound.
Values may be sent and summed in bfloat16 or wider, within the bound.
A program may use at most 64 MiB of HBM per device.

```python
import math
import jax
import jax.numpy as jnp
from jax import lax

D = 2048
HEADS = 32
KV_HEADS = 8
HD = 64
GRID_W = 64
TOK_DEV = 128
TOKENS = 2048
N_TP = 2


def draw_tokens_in(key, part):
    noise_key = jax.random.fold_in(key, 11)
    shift_key = jax.random.fold_in(key, 12)
    dir_key = jax.random.fold_in(key, 13)
    noise = jnp.clip(jax.random.normal(noise_key, (TOKENS, D), jnp.float32), -4.0, 4.0)
    shifts = jax.random.uniform(shift_key, (TOKENS // TOK_DEV, 1), jnp.float32, -1.5, 1.5)
    direction = jnp.clip(jax.random.normal(dir_key, (1, D), jnp.float32), -3.0, 3.0)
    offsets = jnp.repeat(shifts, TOK_DEV, axis=0) * direction
    return (noise + offsets).astype(jnp.bfloat16)


def gain_draw(key):
    return 1.0 + 0.18 * jnp.clip(jax.random.normal(key, (HD,), jnp.float32), -4.0, 4.0)


def draw_q_gain(key, part):
    return gain_draw(jax.random.fold_in(key, 21))


def draw_k_gain(key, part):
    return gain_draw(jax.random.fold_in(key, 22))


def block_levels(own_key, shape, pieces, least, top_value):
    def one(dim, blocks):
        steps = jax.random.uniform(jax.random.fold_in(jax.random.fold_in(own_key, 6), dim), (blocks,), jnp.float32, least / len(pieces), top_value / len(pieces))
        return jnp.repeat(jnp.exp(steps), shape[dim] // blocks).reshape((-1,) + (1,) * (len(shape) - dim - 1))

    level = one(*pieces[0])
    for cut in pieces[1:]:
        level = level * one(*cut)
    return level


def gaussian(rng, dims, scale, bound, cuts=(), kind=jnp.bfloat16):
    values = jax.random.normal(rng, dims, jnp.float32) * scale
    if len(cuts) > 0:
        values = block_levels(rng, dims, cuts, -0.22, 0.18) * values
    return jnp.clip(values, min=-bound, max=bound).astype(kind)


def setup_inputs(seed: int = 0) -> dict:
    key_of = jax.random.split(jax.random.key(seed), 8)
    tokens_in = draw_tokens_in(jax.random.fold_in(key_of[7], 71), 0)
    w_query = gaussian(key_of[1], (D, HEADS * HD), D ** -0.5, 0.125, ((1, 2),))
    w_key = gaussian(key_of[2], (D, KV_HEADS * HD), D ** -0.5, 0.125, ((1, 2),))
    w_value = gaussian(key_of[3], (D, KV_HEADS * HD), D ** -0.5, 0.125, ((1, 2),))
    w_out = gaussian(key_of[4], (HEADS * HD, D), (HEADS * HD) ** -0.5, 0.125, ((0, 2),))
    q_gain = draw_q_gain(jax.random.fold_in(key_of[7], 71), 0)
    k_gain = draw_k_gain(jax.random.fold_in(key_of[7], 71), 0)
    return {"tokens_in": tokens_in, "w_query": w_query, "w_key": w_key, "w_value": w_value, "w_out": w_out, "q_gain": q_gain, "k_gain": k_gain}


def turned(vectors, position, gain):
    pairs = vectors.shape[-1] // 4
    scaled = vectors * lax.rsqrt(lax.optimization_barrier(jnp.mean(vectors * vectors, axis=-1, keepdims=True)) + 1e-06) * gain
    freq = 10000.0 ** (-jnp.arange(pairs, dtype=jnp.float32) / pairs)
    grid_row = (position // GRID_W).astype(jnp.float32)
    grid_col = (position % GRID_W).astype(jnp.float32)
    angle = jnp.stack([grid_row[:, None] * freq, grid_col[:, None] * freq], axis=1)
    cosine = jnp.cos(angle)[:, None]
    sine = jnp.sin(angle)[:, None]
    split = scaled.reshape(scaled.shape[:-1] + (2, 2, pairs))
    first = split[..., 0, :]
    second = split[..., 1, :]
    joined = jnp.stack([first * cosine - second * sine, first * sine + second * cosine], axis=-2)
    return joined.reshape(scaled.shape)

def reference(tokens_in, w_query, w_key, w_value, w_out, q_gain, k_gain):
    head_dim = q_gain.shape[0]
    query = jnp.dot(tokens_in, w_query, preferred_element_type=jnp.float32).astype(jnp.bfloat16)
    key = jnp.dot(tokens_in, w_key, preferred_element_type=jnp.float32).astype(jnp.bfloat16)
    value = jnp.dot(tokens_in, w_value, preferred_element_type=jnp.float32).astype(jnp.bfloat16)
    position = jnp.arange(TOKENS, dtype=jnp.int32)
    group = HEADS // KV_HEADS
    query_n = turned(query.astype(jnp.float32).reshape(TOKENS, HEADS, head_dim), position, q_gain).astype(jnp.bfloat16)
    key_n = turned(key.astype(jnp.float32).reshape(TOKENS, KV_HEADS, head_dim), position, k_gain).astype(jnp.bfloat16)
    value_h = value.reshape(TOKENS, KV_HEADS, head_dim)
    block = math.gcd(TOKENS, 512)
    query_g = query_n.reshape(TOKENS // block, block, KV_HEADS, group, head_dim).transpose(2, 0, 3, 1, 4)
    keys_h = key_n.transpose(1, 0, 2)
    values_h = value_h.transpose(1, 0, 2)

    def one_head(packed):
        queries, keys, values = packed
        keys_f = keys.astype(jnp.float32)
        values_f = values.astype(jnp.float32)

        def one_block(qblock):
            scores = jnp.einsum('gqd,kd->gqk', qblock.astype(jnp.float32), keys_f) * head_dim ** (-0.5)
            peak = lax.optimization_barrier(jnp.max(scores, axis=-1, keepdims=True))
            expo = jnp.exp(scores - peak)
            total = lax.optimization_barrier(jnp.sum(expo, axis=-1, keepdims=True))
            weights = expo.astype(jnp.bfloat16).astype(jnp.float32)
            return (jnp.einsum('gqk,kd->gqd', weights, values_f) / total).astype(jnp.bfloat16)
        return lax.map(one_block, queries)
    mixed = lax.map(one_head, (query_g, keys_h, values_h))
    mixed = mixed.transpose(1, 3, 0, 2, 4).reshape(TOKENS, HEADS * head_dim)
    width = HEADS * head_dim // N_TP
    summed = jnp.zeros((TOKENS, w_out.shape[1]), jnp.float32)
    for index in range(N_TP):
        partial_value = jnp.dot(mixed[:, index * width:(index + 1) * width], w_out[index * width:(index + 1) * width], preferred_element_type=jnp.float32).astype(jnp.bfloat16)
        partial_value = lax.optimization_barrier(partial_value)
        summed = summed + partial_value.astype(jnp.float32)
    return summed.astype(jnp.bfloat16)
```

```python
import functools

import jax
import jax.numpy as jnp
import numpy as np
from jax import lax
from jax.experimental import pallas as pl
from jax.experimental.pallas import tpu as pltpu
from jax.sharding import PartitionSpec as P

GRID_W = 64
LANES = 128


def tables(token_count, head_dim):
    pairs = head_dim // 4
    lane = np.arange(LANES)
    freq = 10000.0 ** (-(lane % pairs) / pairs)
    sign = np.where(lane % (2 * pairs) < pairs, -1.0, 1.0)

    def both(count):
        angle = np.arange(count)[:, None] * freq[None, :]
        return np.concatenate([np.cos(angle), np.sin(angle) * sign], axis=1).astype(np.float32)

    return both(token_count // GRID_W), both(GRID_W)


def kernel(
    n_sp, n_tp, members, head_dim,
    tok_hbm, wq_hbm, wkv_hbms, wo_hbm, row_ref, col_ref, qg_ref, kg_ref, out_ref,
    x, wq, wkvs, wo, kv_out, kv_all, q_out, q_all, qm, k4, v1, peak, acc, m_out, m_all, o_acc, o_out, o_in,
    load_sem, x_send, x_recv, kv_send, kv_recv, q_send, q_recv, m_send, m_recv, o_send, o_recv,
):
    sp, tp = lax.axis_index("sp"), lax.axis_index("tp")
    own_rows = tok_hbm.shape[0]
    rows = own_rows * n_tp
    groups = n_sp // members
    plane, member = sp // members, sp % members
    query_cols = wq.shape[1]
    width = query_cols // members
    heads = width // head_dim
    first = plane * members

    def sp_copy(src, dst, send, recv, to):
        return pltpu.make_async_remote_copy(
            src_ref=src, dst_ref=dst, send_sem=send, recv_sem=recv,
            device_id={"sp": to}, device_id_type=pl.DeviceIdType.MESH)

    def tp_copy(src, dst, send, recv, to):
        return pltpu.make_async_remote_copy(
            src_ref=src, dst_ref=dst, send_sem=send, recv_sem=recv,
            device_id={"tp": to}, device_id_type=pl.DeviceIdType.MESH)

    def own_slice(index):
        return pl.ds(pl.multiple_of(index * own_rows, own_rows), own_rows)

    loads = [pltpu.make_async_copy(tok_hbm, x.at[own_slice(tp)], load_sem.at[0])]
    for i, (src, dst) in enumerate(zip((*wkv_hbms, wq_hbm, wo_hbm), (*wkvs, wq, wo))):
        loads.append(pltpu.make_async_copy(src, dst, load_sem.at[i + 1]))
    for load in loads:
        load.start()
    barrier = pltpu.get_barrier_semaphore()
    for step in range(1, n_tp):
        pl.semaphore_signal(barrier, inc=1, device_id={"tp": (tp + step) % n_tp}, device_id_type=pl.DeviceIdType.MESH)

    def greet(step, carry):
        pl.semaphore_signal(barrier, inc=1, device_id={"sp": (sp + step) % n_sp}, device_id_type=pl.DeviceIdType.MESH)
        return carry

    lax.fori_loop(1, n_sp, greet, 0)

    lane = lax.broadcasted_iota(jnp.int32, (rows, LANES), 1)
    low = lane % head_dim < head_dim // 2
    left = lane % (head_dim // 2) < head_dim // 4
    even = lane < head_dim
    cos_parts, sin_parts = [], []
    per_dev = rows // GRID_W
    low_g = low[:GRID_W]
    for i in range(per_dev):
        line = row_ref[pl.ds(sp * per_dev + i, 1), :]
        cos_parts.append(jnp.where(low_g, jnp.broadcast_to(line[:, :LANES], (GRID_W, LANES)), col_ref[:, :LANES]))
        sin_parts.append(jnp.where(low_g, jnp.broadcast_to(line[:, LANES:], (GRID_W, LANES)), col_ref[:, LANES:]))
    cosine = jnp.concatenate(cos_parts, axis=0)
    sine = jnp.concatenate(sin_parts, axis=0)
    ones_r = lax.broadcasted_iota(jnp.int32, (LANES, LANES), 0) // head_dim
    ones_c = lax.broadcasted_iota(jnp.int32, (LANES, LANES), 1) // head_dim
    block = jnp.where(ones_r == ones_c, 1.0, 0.0).astype(jnp.bfloat16)
    gain_q = jnp.concatenate([qg_ref[...]] * (LANES // head_dim), axis=1) * head_dim ** (-0.5)
    gain_k = jnp.concatenate([kg_ref[...]] * (LANES // head_dim), axis=1)

    def turned(u, gain):
        square = u * u
        high = square.astype(jnp.bfloat16)
        rest = (square - high.astype(jnp.float32)).astype(jnp.bfloat16)
        total = jnp.dot(high, block, preferred_element_type=jnp.float32) + jnp.dot(
            rest, block, preferred_element_type=jnp.float32)
        n = u * lax.rsqrt(total * (1.0 / head_dim) + 1e-06) * gain
        quarter = head_dim // 4
        other = jnp.where(left, pltpu.roll(n, LANES - quarter, 1), pltpu.roll(n, quarter, 1))
        return n * cosine + other * sine

    def project(w):
        return jnp.dot(x[...], w, preferred_element_type=jnp.float32).astype(jnp.bfloat16).astype(jnp.float32)

    peak[...] = jnp.full_like(peak, -1e30)
    acc[...] = jnp.zeros_like(acc)

    loads[0].wait()
    pl.semaphore_wait(barrier, n_sp - 1 + n_tp - 1)
    x_copies = []
    for step in range(1, n_tp):
        mine = x.at[own_slice(tp)]
        copy = tp_copy(mine, mine, x_send.at[step], x_recv.at[step], (tp + step) % n_tp)
        copy.start()
        x_copies.append(copy)
    for step in range(1, n_tp):
        theirs = x.at[own_slice((tp + n_tp - step) % n_tp)]
        tp_copy(theirs, theirs, x_send.at[step], x_recv.at[step], (tp + step) % n_tp).wait_recv()

    for i in range(len(wkvs)):
        loads[1 + i].wait()
    if len(wkvs) == 2:
        keys = project(wkvs[0][...])
        vals = project(wkvs[1][...])
        for pair in range(members // 2):
            cut = slice(pair * LANES, (pair + 1) * LANES)
            k, v = turned(keys[:, cut], gain_k), vals[:, cut]
            kv_out[2 * pair] = jnp.where(even, k, pltpu.roll(v, head_dim, 1)).astype(jnp.bfloat16)
            kv_out[2 * pair + 1] = jnp.where(even, pltpu.roll(k, head_dim, 1), v).astype(jnp.bfloat16)
    else:
        both = project(wkvs[0][...])
        kv_out[0] = jnp.where(even, turned(both, gain_k), both).astype(jnp.bfloat16)

    def kv_copy(step):
        to = (sp + step) % n_sp
        return sp_copy(kv_out.at[to % members], kv_all.at[sp], kv_send.at[step], kv_recv.at[sp], to)

    def send_kv(i, carry):
        kv_copy(n_sp - i).start()
        return carry

    lax.fori_loop(1, n_sp, send_kv, 0)
    kv_all[sp] = kv_out[member]

    loads[1 + len(wkvs)].wait()
    for p in range(members):
        u = project(wq[:, p * width:(p + 1) * width])
        for t in range(width // LANES):
            cut = slice(t * LANES, (t + 1) * LANES)
            q_out[p, :, cut] = turned(u[:, cut], gain_q).astype(jnp.bfloat16)

    def q_copy(step):
        to = (member + step) % members
        return sp_copy(q_out.at[to], q_all.at[member], q_send.at[step], q_recv.at[member], first + to)

    for step in range(1, members):
        q_copy(step).start()
    q_all[member] = q_out[member]

    wide_lane = lax.broadcasted_iota(jnp.int32, (rows, width), 1) // head_dim

    def mask_queries(c):
        q = q_all[c]
        for g in range(heads):
            qm[pl.ds(pl.multiple_of((c * heads + g) * rows, rows), rows), :] = jnp.where(
                wide_lane == g, q, jnp.zeros_like(q))

    mask_queries(member)
    for step in range(1, members):
        c = (member + members - step) % members
        sp_copy(q_out.at[c], q_all.at[c], q_send.at[step], q_recv.at[c], first + c).wait_recv()
        mask_queries(c)

    tall = 2 * rows

    def prepare(slot, c):
        tile = kv_all[slot].astype(jnp.float32)
        turned_tile = pltpu.roll(tile, head_dim, 1)
        kk = jnp.where(even, tile, turned_tile).astype(jnp.bfloat16)
        place = pl.ds(c * rows, rows)
        for t in range(width // LANES):
            k4[place, t * LANES:(t + 1) * LANES] = kk
        v1[place, :] = jnp.where(even, turned_tile, 1.0).astype(jnp.bfloat16)

    def wait_kv(slot):
        sp_copy(kv_all.at[slot], kv_all.at[slot], kv_send.at[0], kv_recv.at[slot], sp).wait_recv()

    def attend(c):
        def one(i, carry):
            place = pl.ds(pl.multiple_of(c * heads * rows + i * tall, tall), tall)
            scores = lax.dot_general(qm[place, :], k4[...], (((1,), (1,)), ((), ())),
                                     preferred_element_type=jnp.float32)
            before = peak[place, :]
            now = jnp.maximum(before, jnp.max(scores, axis=1, keepdims=True))
            expo = jnp.exp(scores - jnp.concatenate([now] * (scores.shape[1] // LANES), axis=1))
            peak[place, :] = now
            acc[place, :] = acc[place, :] * jnp.exp(before - now) + jnp.dot(
                expo.astype(jnp.bfloat16), v1[...], preferred_element_type=jnp.float32)
            return carry

        lax.fori_loop(0, heads // 2, one, 0, unroll=True)

    def finish(c):
        parts = []
        for pair in range(heads // 2):
            halves = []
            for g in (2 * pair, 2 * pair + 1):
                piece = acc[pl.ds(pl.multiple_of((c * heads + g) * rows, rows), rows), :]
                halves.append(piece / pltpu.roll(piece, head_dim, 1))
            parts.append(jnp.where(even, halves[0], pltpu.roll(halves[1], head_dim, 1)))
        m_out[c] = jnp.concatenate(parts, axis=1).astype(jnp.bfloat16)

    def m_copy(step):
        to = (member + step) % members
        return sp_copy(m_out.at[to], m_all.at[member], m_send.at[step], m_recv.at[member], first + to)

    for step in range(1, members):
        wait_kv(first + (member + step) % members)
    for c in range(members):
        prepare(first + c, c)

    def whole_group(d, carry):
        base = ((plane + d) % groups) * members

        @pl.when(d > 0)
        def _():
            for c in range(members):
                wait_kv(base + c)
                prepare(base + c, c)

        def per(c, inner):
            attend(c)
            return inner

        lax.fori_loop(0, members, per, 0)
        return carry

    lax.fori_loop(0, groups - 1, whole_group, 0)
    last = ((plane + groups - 1) % groups) * members
    for c in range(members):
        wait_kv(last + c)
        prepare(last + c, c)
    for step in range(1, members + 1):
        c = (member + step) % members
        attend(c)
        finish(c)
        if step < members:
            m_copy(step).start()
    m_all[member] = m_out[member]

    loads[2 + len(wkvs)].wait()
    for step in range(members):
        s = (member + members - step) % members
        if step:
            sp_copy(m_out.at[s], m_all.at[s], m_send.at[step], m_recv.at[s], first + s).wait_recv()
        term = jnp.dot(m_all[s], wo[pl.ds(pl.multiple_of(s * width, width), width), :],
                       preferred_element_type=jnp.float32)
        if step == 0:
            o_acc[...] = term
        else:
            o_acc[...] += term
    o_copies = []
    for step in range(1, n_tp):
        to = (tp + step) % n_tp
        o_out[step] = o_acc[own_slice(to), :].astype(jnp.bfloat16)
        copy = tp_copy(o_out.at[step], o_in.at[step], o_send.at[step], o_recv.at[step], to)
        copy.start()
        o_copies.append(copy)
    result = o_acc[own_slice(tp), :].astype(jnp.bfloat16).astype(jnp.float32)
    for step in range(1, n_tp):
        o_copies[step - 1].wait_recv()
        result = result + o_in[step].astype(jnp.float32)
    out_ref[...] = result.astype(jnp.bfloat16)

    for copy in x_copies + o_copies:
        copy.wait_send()
    for step in range(1, members):
        q_copy(step).wait_send()
        m_copy(step).wait_send()

    def sent_kv(step, carry):
        kv_copy(step).wait_send()
        return carry

    lax.fori_loop(1, n_sp, sent_kv, 0)


def solution(mesh):
    n_sp, n_tp = mesh.shape["sp"], mesh.shape["tp"]

    def body(tokens_in, w_query, w_key, w_value, w_out, q_gain, k_gain):
        head_dim = q_gain.shape[0]
        own_rows, depth = tokens_in.shape
        rows = own_rows * n_tp
        query_cols, key_cols = w_query.shape[1], w_key.shape[1]
        members = key_cols // head_dim
        width = query_cols // members
        heads = width // head_dim
        if key_cols % LANES:
            wkv = (jnp.concatenate([w_key, w_value], axis=1),)
        else:
            wkv = (w_key, w_value)
        row_table, col_table = tables(rows * n_sp, head_dim)
        bf, f32 = jnp.bfloat16, jnp.float32
        hbm = pl.BlockSpec(memory_space=pltpu.HBM)
        vmem = pl.BlockSpec(memory_space=pltpu.VMEM)
        dma = pltpu.SemaphoreType.DMA
        call = pl.pallas_call(
            functools.partial(kernel, n_sp, n_tp, members, head_dim),
            out_shape=jax.ShapeDtypeStruct((own_rows, w_out.shape[1]), bf),
            in_specs=[hbm, hbm, (hbm,) * len(wkv), hbm, vmem, vmem, vmem, vmem],
            out_specs=vmem,
            scratch_shapes=[
                pltpu.VMEM((rows, depth), bf),
                pltpu.VMEM(w_query.shape, bf),
                tuple(pltpu.VMEM(w.shape, bf) for w in wkv),
                pltpu.VMEM(w_out.shape, bf),
                pltpu.VMEM((members, rows, LANES), bf),
                pltpu.VMEM((n_sp, rows, LANES), bf),
                pltpu.VMEM((members, rows, width), bf),
                pltpu.VMEM((members, rows, width), bf),
                pltpu.VMEM((members * heads * rows, width), bf),
                pltpu.VMEM((members * rows, width), bf),
                pltpu.VMEM((members * rows, LANES), bf),
                pltpu.VMEM((members * heads * rows, LANES), f32),
                pltpu.VMEM((members * heads * rows, LANES), f32),
                pltpu.VMEM((members, rows, width), bf),
                pltpu.VMEM((members, rows, width), bf),
                pltpu.VMEM((rows, w_out.shape[1]), f32),
                pltpu.VMEM((n_tp, own_rows, w_out.shape[1]), bf),
                pltpu.VMEM((n_tp, own_rows, w_out.shape[1]), bf),
                dma((6,)),
                dma((n_tp,)), dma((n_tp,)),
                dma((n_sp,)), dma((n_sp,)),
                dma((members,)), dma((members,)),
                dma((members,)), dma((members,)),
                dma((n_tp,)), dma((n_tp,)),
            ],
            compiler_params=pltpu.CompilerParams(
                collective_id=0, has_side_effects=True, vmem_limit_bytes=56 * 1024 * 1024),
        )
        return call(tokens_in, w_query, wkv, w_out, jnp.asarray(row_table), jnp.asarray(col_table),
                    q_gain.reshape(1, head_dim), k_gain.reshape(1, head_dim))

    return jax.shard_map(
        body,
        mesh=mesh,
        in_specs=(
            P(("sp", "tp"), None),
            P(None, "tp"),
            P(None, "tp"),
            P(None, "tp"),
            P("tp", None),
            P(),
            P(),
        ),
        out_specs=P(("sp", "tp"), None),
        check_vma=False,
    )
```

```python
import functools

import jax
import jax.numpy as jnp
import numpy as np
from jax import lax
from jax.experimental import pallas as pl
from jax.experimental.pallas import tpu as pltpu
from jax.sharding import PartitionSpec as P

GRID_W = 64
LANES = 128


def tables(token_count, head_dim):
    pairs = head_dim // 4
    lane = np.arange(LANES)
    freq = 10000.0 ** (-(lane % pairs) / pairs)
    sign = np.where(lane % (2 * pairs) < pairs, -1.0, 1.0)

    def both(count):
        angle = np.arange(count)[:, None] * freq[None, :]
        return np.concatenate([np.cos(angle), np.sin(angle) * sign], axis=1).astype(np.float32)

    return both(token_count // GRID_W), both(GRID_W)


def kernel(
    n_sp, n_tp, members, head_dim,
    tok_hbm, wq_hbm, wkv_hbms, wo_hbm, row_ref, col_ref, qg_ref, kg_ref, out_ref,
    x, wq, wkvs, wo, kv_out, kv_all, q_out, q_all, qm, k4, v1, peak, acc, m_out, m_all, o_acc, o_out, o_in,
    load_sem, x_send, x_recv, kv_send, kv_recv, line_send, q_send, q_recv, m_send, m_recv, o_send, o_recv,
):
    sp, tp = lax.axis_index("sp"), lax.axis_index("tp")
    own_rows = tok_hbm.shape[0]
    rows = own_rows * n_tp
    groups = n_sp // members
    plane, member = sp // members, sp % members
    query_cols = wq.shape[1]
    width = query_cols // members
    heads = width // head_dim
    first = plane * members

    def sp_copy(src, dst, send, recv, to):
        return pltpu.make_async_remote_copy(
            src_ref=src, dst_ref=dst, send_sem=send, recv_sem=recv,
            device_id={"sp": to}, device_id_type=pl.DeviceIdType.MESH)

    def tp_copy(src, dst, send, recv, to):
        return pltpu.make_async_remote_copy(
            src_ref=src, dst_ref=dst, send_sem=send, recv_sem=recv,
            device_id={"tp": to}, device_id_type=pl.DeviceIdType.MESH)

    def own_slice(index):
        return pl.ds(pl.multiple_of(index * own_rows, own_rows), own_rows)

    loads = [pltpu.make_async_copy(tok_hbm, x.at[own_slice(tp)], load_sem.at[0])]
    for i, (src, dst) in enumerate(zip((*wkv_hbms, wq_hbm, wo_hbm), (*wkvs, wq, wo))):
        loads.append(pltpu.make_async_copy(src, dst, load_sem.at[i + 1]))
    for load in loads:
        load.start()
    barrier = pltpu.get_barrier_semaphore()
    for step in range(1, n_tp):
        pl.semaphore_signal(barrier, inc=1, device_id={"tp": (tp + step) % n_tp}, device_id_type=pl.DeviceIdType.MESH)

    for step in range(1, members):
        pl.semaphore_signal(barrier, inc=1, device_id={"sp": first + (member + step) % members},
                            device_id_type=pl.DeviceIdType.MESH)

    def greet(step, carry):
        pl.semaphore_signal(barrier, inc=1, device_id={"sp": (sp + step * members) % n_sp},
                            device_id_type=pl.DeviceIdType.MESH)
        return carry

    lax.fori_loop(1, groups, greet, 0)

    lane = lax.broadcasted_iota(jnp.int32, (rows, LANES), 1)
    low = lane % head_dim < head_dim // 2
    left = lane % (head_dim // 2) < head_dim // 4
    even = lane < head_dim
    cos_parts, sin_parts = [], []
    per_dev = rows // GRID_W
    low_g = low[:GRID_W]
    for i in range(per_dev):
        line = row_ref[pl.ds(sp * per_dev + i, 1), :]
        cos_parts.append(jnp.where(low_g, jnp.broadcast_to(line[:, :LANES], (GRID_W, LANES)), col_ref[:, :LANES]))
        sin_parts.append(jnp.where(low_g, jnp.broadcast_to(line[:, LANES:], (GRID_W, LANES)), col_ref[:, LANES:]))
    cosine = jnp.concatenate(cos_parts, axis=0)
    sine = jnp.concatenate(sin_parts, axis=0)
    ones_r = lax.broadcasted_iota(jnp.int32, (LANES, LANES), 0) // head_dim
    ones_c = lax.broadcasted_iota(jnp.int32, (LANES, LANES), 1) // head_dim
    block = jnp.where(ones_r == ones_c, 1.0, 0.0).astype(jnp.bfloat16)
    gain_q = jnp.concatenate([qg_ref[...]] * (LANES // head_dim), axis=1) * head_dim ** (-0.5)
    gain_k = jnp.concatenate([kg_ref[...]] * (LANES // head_dim), axis=1)

    def turned(u, gain):
        square = u * u
        high = square.astype(jnp.bfloat16)
        rest = (square - high.astype(jnp.float32)).astype(jnp.bfloat16)
        total = jnp.dot(high, block, preferred_element_type=jnp.float32) + jnp.dot(
            rest, block, preferred_element_type=jnp.float32)
        n = u * lax.rsqrt(total * (1.0 / head_dim) + 1e-06) * gain
        quarter = head_dim // 4
        other = jnp.where(left, pltpu.roll(n, LANES - quarter, 1), pltpu.roll(n, quarter, 1))
        return n * cosine + other * sine

    def project(w):
        return jnp.dot(x[...], w, preferred_element_type=jnp.float32).astype(jnp.bfloat16).astype(jnp.float32)

    peak[...] = jnp.full_like(peak, -1e30)
    acc[...] = jnp.zeros_like(acc)

    loads[0].wait()
    pl.semaphore_wait(barrier, groups - 1 + members - 1 + n_tp - 1)
    x_copies = []
    for step in range(1, n_tp):
        mine = x.at[own_slice(tp)]
        copy = tp_copy(mine, mine, x_send.at[step], x_recv.at[step], (tp + step) % n_tp)
        copy.start()
        x_copies.append(copy)
    for step in range(1, n_tp):
        theirs = x.at[own_slice((tp + n_tp - step) % n_tp)]
        tp_copy(theirs, theirs, x_send.at[step], x_recv.at[step], (tp + step) % n_tp).wait_recv()

    for i in range(len(wkvs)):
        loads[1 + i].wait()
    if len(wkvs) == 2:
        keys = project(wkvs[0][...])
        vals = project(wkvs[1][...])
        for pair in range(members // 2):
            cut = slice(pair * LANES, (pair + 1) * LANES)
            k, v = turned(keys[:, cut], gain_k), vals[:, cut]
            kv_out[2 * pair] = jnp.where(even, k, pltpu.roll(v, head_dim, 1)).astype(jnp.bfloat16)
            kv_out[2 * pair + 1] = jnp.where(even, pltpu.roll(k, head_dim, 1), v).astype(jnp.bfloat16)
    else:
        both = project(wkvs[0][...])
        kv_out[0] = jnp.where(even, turned(both, gain_k), both).astype(jnp.bfloat16)

    kv_all[sp] = kv_out[member]

    def kv_copy(step):
        to = (member + step) % members
        return sp_copy(kv_out.at[to], kv_all.at[sp], kv_send.at[step], kv_recv.at[sp], first + to)

    for step in range(1, members):
        kv_copy(step).start()

    below, above = plane, groups - 1 - plane
    both_sides = jnp.minimum(below, above)

    def nearest(i):
        distance = jnp.where(i <= 2 * both_sides, (i + 1) // 2, i - both_sides)
        upward = jnp.where(i <= 2 * both_sides, i % 2, jnp.where(above > below, 1, 0))
        return plane + distance * (2 * upward - 1)

    def line_copy(i, c):
        slot = kv_all.at[first + c]
        return sp_copy(slot, slot, line_send.at[i * members + c], kv_recv.at[first + c], nearest(i) * members + member)

    def wait_kv(slot):
        sp_copy(kv_all.at[slot], kv_all.at[slot], kv_send.at[0], kv_recv.at[slot], sp).wait_recv()

    loads[1 + len(wkvs)].wait()
    for p in range(members):
        u = project(wq[:, p * width:(p + 1) * width])
        for t in range(width // LANES):
            cut = slice(t * LANES, (t + 1) * LANES)
            q_out[p, :, cut] = turned(u[:, cut], gain_q).astype(jnp.bfloat16)

    def q_copy(step):
        to = (member + step) % members
        return sp_copy(q_out.at[to], q_all.at[member], q_send.at[step], q_recv.at[member], first + to)

    for step in range(1, members):
        q_copy(step).start()
    q_all[member] = q_out[member]

    for step in range(1, members):
        wait_kv(first + (member + members - step) % members)

    def along(i, carry):
        for c in range(members):
            line_copy(i, c).start()
        return carry

    lax.fori_loop(1, groups, along, 0)

    wide_lane = lax.broadcasted_iota(jnp.int32, (rows, width), 1) // head_dim

    def mask_queries(c):
        q = q_all[c]
        for g in range(heads):
            qm[pl.ds(pl.multiple_of((c * heads + g) * rows, rows), rows), :] = jnp.where(
                wide_lane == g, q, jnp.zeros_like(q))

    tall = heads * rows

    def prepare(slot, c):
        tile = kv_all[slot].astype(jnp.float32)
        turned_tile = pltpu.roll(tile, head_dim, 1)
        kk = jnp.where(even, tile, turned_tile).astype(jnp.bfloat16)
        place = pl.ds(c * rows, rows)
        for t in range(width // LANES):
            k4[place, t * LANES:(t + 1) * LANES] = kk
        v1[place, :] = jnp.where(even, turned_tile, 1.0).astype(jnp.bfloat16)

    def attend(c):
        place = pl.ds(pl.multiple_of(c * tall, tall), tall)
        scores = lax.dot_general(qm[place, :], k4[...], (((1,), (1,)), ((), ())),
                                 preferred_element_type=jnp.float32)
        before = peak[place, :]
        now = jnp.maximum(before, jnp.max(scores, axis=1, keepdims=True))
        expo = jnp.exp(scores - jnp.concatenate([now] * (scores.shape[1] // LANES), axis=1))
        peak[place, :] = now
        acc[place, :] = acc[place, :] * jnp.exp(before - now) + jnp.dot(
            expo.astype(jnp.bfloat16), v1[...], preferred_element_type=jnp.float32)

    def finish(c):
        parts = []
        for pair in range(heads // 2):
            halves = []
            for g in (2 * pair, 2 * pair + 1):
                piece = acc[pl.ds(pl.multiple_of((c * heads + g) * rows, rows), rows), :]
                halves.append(piece / pltpu.roll(piece, head_dim, 1))
            parts.append(jnp.where(even, halves[0], pltpu.roll(halves[1], head_dim, 1)))
        m_out[c] = jnp.concatenate(parts, axis=1).astype(jnp.bfloat16)

    def m_copy(step):
        to = (member + step) % members
        return sp_copy(m_out.at[to], m_all.at[member], m_send.at[step], m_recv.at[member], first + to)

    for c in range(members):
        prepare(first + c, c)
    for step in range(members):
        c = (member + members - step) % members
        if step:
            sp_copy(q_out.at[c], q_all.at[c], q_send.at[step], q_recv.at[c], first + c).wait_recv()
        mask_queries(c)
        attend(c)

    def fetch(i):
        base = nearest(i) * members
        for c in range(members):
            wait_kv(base + c)
            prepare(base + c, c)

    def whole_group(i, carry):
        fetch(i)
        for c in range(members):
            attend(c)
        return carry

    lax.fori_loop(1, groups - 1, whole_group, 0)
    fetch(groups - 1)
    for step in range(1, members + 1):
        c = (member + step) % members
        attend(c)
        finish(c)
        if step < members:
            m_copy(step).start()
    m_all[member] = m_out[member]

    loads[2 + len(wkvs)].wait()
    for step in range(members):
        s = (member + members - step) % members
        if step:
            sp_copy(m_out.at[s], m_all.at[s], m_send.at[step], m_recv.at[s], first + s).wait_recv()
        term = jnp.dot(m_all[s], wo[pl.ds(pl.multiple_of(s * width, width), width), :],
                       preferred_element_type=jnp.float32)
        if step == 0:
            o_acc[...] = term
        else:
            o_acc[...] += term
    o_copies = []
    for step in range(1, n_tp):
        to = (tp + step) % n_tp
        o_out[step] = o_acc[own_slice(to), :].astype(jnp.bfloat16)
        copy = tp_copy(o_out.at[step], o_in.at[step], o_send.at[step], o_recv.at[step], to)
        copy.start()
        o_copies.append(copy)
    result = o_acc[own_slice(tp), :].astype(jnp.bfloat16).astype(jnp.float32)
    for step in range(1, n_tp):
        o_copies[step - 1].wait_recv()
        result = result + o_in[step].astype(jnp.float32)
    out_ref[...] = result.astype(jnp.bfloat16)

    for copy in x_copies + o_copies:
        copy.wait_send()
    for step in range(1, members):
        kv_copy(step).wait_send()
        q_copy(step).wait_send()
        m_copy(step).wait_send()

    def sent_along(i, carry):
        for c in range(members):
            line_copy(i, c).wait_send()
        return carry

    lax.fori_loop(1, groups, sent_along, 0)


def solution(mesh):
    n_sp, n_tp = mesh.shape["sp"], mesh.shape["tp"]

    def body(tokens_in, w_query, w_key, w_value, w_out, q_gain, k_gain):
        head_dim = q_gain.shape[0]
        own_rows, depth = tokens_in.shape
        rows = own_rows * n_tp
        query_cols, key_cols = w_query.shape[1], w_key.shape[1]
        members = key_cols // head_dim
        width = query_cols // members
        heads = width // head_dim
        if key_cols % LANES:
            wkv = (jnp.concatenate([w_key, w_value], axis=1),)
        else:
            wkv = (w_key, w_value)
        row_table, col_table = tables(rows * n_sp, head_dim)
        bf, f32 = jnp.bfloat16, jnp.float32
        hbm = pl.BlockSpec(memory_space=pltpu.HBM)
        vmem = pl.BlockSpec(memory_space=pltpu.VMEM)
        dma = pltpu.SemaphoreType.DMA
        call = pl.pallas_call(
            functools.partial(kernel, n_sp, n_tp, members, head_dim),
            out_shape=jax.ShapeDtypeStruct((own_rows, w_out.shape[1]), bf),
            in_specs=[hbm, hbm, (hbm,) * len(wkv), hbm, vmem, vmem, vmem, vmem],
            out_specs=vmem,
            scratch_shapes=[
                pltpu.VMEM((rows, depth), bf),
                pltpu.VMEM(w_query.shape, bf),
                tuple(pltpu.VMEM(w.shape, bf) for w in wkv),
                pltpu.VMEM(w_out.shape, bf),
                pltpu.VMEM((members, rows, LANES), bf),
                pltpu.VMEM((n_sp, rows, LANES), bf),
                pltpu.VMEM((members, rows, width), bf),
                pltpu.VMEM((members, rows, width), bf),
                pltpu.VMEM((members * heads * rows, width), bf),
                pltpu.VMEM((members * rows, width), bf),
                pltpu.VMEM((members * rows, LANES), bf),
                pltpu.VMEM((members * heads * rows, LANES), f32),
                pltpu.VMEM((members * heads * rows, LANES), f32),
                pltpu.VMEM((members, rows, width), bf),
                pltpu.VMEM((members, rows, width), bf),
                pltpu.VMEM((rows, w_out.shape[1]), f32),
                pltpu.VMEM((n_tp, own_rows, w_out.shape[1]), bf),
                pltpu.VMEM((n_tp, own_rows, w_out.shape[1]), bf),
                dma((6,)),
                dma((n_tp,)), dma((n_tp,)),
                dma((members,)), dma((n_sp,)), dma((n_sp,)),
                dma((members,)), dma((members,)),
                dma((members,)), dma((members,)),
                dma((n_tp,)), dma((n_tp,)),
            ],
            compiler_params=pltpu.CompilerParams(
                collective_id=0, has_side_effects=True, vmem_limit_bytes=56 * 1024 * 1024),
        )
        return call(tokens_in, w_query, wkv, w_out, jnp.asarray(row_table), jnp.asarray(col_table),
                    q_gain.reshape(1, head_dim), k_gain.reshape(1, head_dim))

    return jax.shard_map(
        body,
        mesh=mesh,
        in_specs=(
            P(("sp", "tp"), None),
            P(None, "tp"),
            P(None, "tp"),
            P(None, "tp"),
            P("tp", None),
            P(),
            P(),
        ),
        out_specs=P(("sp", "tp"), None),
        check_vma=False,
    )
```

```python
import functools

import jax
import jax.numpy as jnp
import numpy as np
from jax import lax
from jax.experimental import pallas as pl
from jax.experimental.pallas import tpu as pltpu
from jax.sharding import PartitionSpec as P

GRID_W = 64
LANES = 128
REACH = 2


def tables(token_count, head_dim):
    pairs = head_dim // 4
    lane = np.arange(LANES)
    freq = 10000.0 ** (-(lane % pairs) / pairs)
    sign = np.where(lane % (2 * pairs) < pairs, -1.0, 1.0)

    def both(count):
        angle = np.arange(count)[:, None] * freq[None, :]
        return np.concatenate([np.cos(angle), np.sin(angle) * sign], axis=1).astype(np.float32)

    return both(token_count // GRID_W), both(GRID_W)


def kernel(
    n_sp, n_tp, members, head_dim,
    tok_hbm, wq_hbm, wkv_hbms, wo_hbm, row_ref, col_ref, qg_ref, kg_ref, out_ref,
    x, wq, wkvs, wo, kv_out, kv_all, q_out, q_all, qm, k4, v1, peak, acc, m_out, m_all, o_acc, o_out, o_in,
    load_sem, x_send, x_recv, kv_send, kv_recv, line_send, on_send, q_send, q_recv, m_send, m_recv, o_send, o_recv,
):
    sp, tp = lax.axis_index("sp"), lax.axis_index("tp")
    own_rows = tok_hbm.shape[0]
    rows = own_rows * n_tp
    groups = n_sp // members
    plane, member = sp // members, sp % members
    query_cols = wq.shape[1]
    width = query_cols // members
    heads = width // head_dim
    first = plane * members

    def sp_copy(src, dst, send, recv, to):
        return pltpu.make_async_remote_copy(
            src_ref=src, dst_ref=dst, send_sem=send, recv_sem=recv,
            device_id={"sp": to}, device_id_type=pl.DeviceIdType.MESH)

    def tp_copy(src, dst, send, recv, to):
        return pltpu.make_async_remote_copy(
            src_ref=src, dst_ref=dst, send_sem=send, recv_sem=recv,
            device_id={"tp": to}, device_id_type=pl.DeviceIdType.MESH)

    def own_slice(index):
        return pl.ds(pl.multiple_of(index * own_rows, own_rows), own_rows)

    below, above = plane, groups - 1 - plane
    both_sides = jnp.minimum(below, above)

    def way(i):
        paired = i <= 2 * both_sides
        distance = jnp.where(paired, (i + 1) // 2, i - both_sides)
        upward = jnp.where(paired, i % 2, jnp.where(above > below, 1, 0))
        return distance, 2 * upward - 1

    def nearest(i):
        distance, side = way(i)
        return plane + distance * side

    loads = [pltpu.make_async_copy(tok_hbm, x.at[own_slice(tp)], load_sem.at[0])]
    for i, (src, dst) in enumerate(zip((*wkv_hbms, wq_hbm, wo_hbm), (*wkvs, wq, wo))):
        loads.append(pltpu.make_async_copy(src, dst, load_sem.at[i + 1]))
    for load in loads:
        load.start()
    barrier = pltpu.get_barrier_semaphore()
    for step in range(1, n_tp):
        pl.semaphore_signal(barrier, inc=1, device_id={"tp": (tp + step) % n_tp}, device_id_type=pl.DeviceIdType.MESH)

    for step in range(1, members):
        pl.semaphore_signal(barrier, inc=1, device_id={"sp": first + (member + step) % members},
                            device_id_type=pl.DeviceIdType.MESH)

    def greet(i, carry):
        @pl.when(way(i)[0] <= REACH)
        def _():
            pl.semaphore_signal(barrier, inc=1, device_id={"sp": nearest(i) * members + member},
                                device_id_type=pl.DeviceIdType.MESH)
        return carry

    lax.fori_loop(1, groups, greet, 0)

    lane = lax.broadcasted_iota(jnp.int32, (rows, LANES), 1)
    low = lane % head_dim < head_dim // 2
    left = lane % (head_dim // 2) < head_dim // 4
    even = lane < head_dim
    cos_parts, sin_parts = [], []
    per_dev = rows // GRID_W
    low_g = low[:GRID_W]
    for i in range(per_dev):
        line = row_ref[pl.ds(sp * per_dev + i, 1), :]
        cos_parts.append(jnp.where(low_g, jnp.broadcast_to(line[:, :LANES], (GRID_W, LANES)), col_ref[:, :LANES]))
        sin_parts.append(jnp.where(low_g, jnp.broadcast_to(line[:, LANES:], (GRID_W, LANES)), col_ref[:, LANES:]))
    cosine = jnp.concatenate(cos_parts, axis=0)
    sine = jnp.concatenate(sin_parts, axis=0)
    ones_r = lax.broadcasted_iota(jnp.int32, (LANES, LANES), 0) // head_dim
    ones_c = lax.broadcasted_iota(jnp.int32, (LANES, LANES), 1) // head_dim
    block = jnp.where(ones_r == ones_c, 1.0, 0.0).astype(jnp.bfloat16)
    gain_q = jnp.concatenate([qg_ref[...]] * (LANES // head_dim), axis=1) * head_dim ** (-0.5)
    gain_k = jnp.concatenate([kg_ref[...]] * (LANES // head_dim), axis=1)

    def turned(u, gain):
        square = u * u
        high = square.astype(jnp.bfloat16)
        rest = (square - high.astype(jnp.float32)).astype(jnp.bfloat16)
        total = jnp.dot(high, block, preferred_element_type=jnp.float32) + jnp.dot(
            rest, block, preferred_element_type=jnp.float32)
        n = u * lax.rsqrt(total * (1.0 / head_dim) + 1e-06) * gain
        quarter = head_dim // 4
        other = jnp.where(left, pltpu.roll(n, LANES - quarter, 1), pltpu.roll(n, quarter, 1))
        return n * cosine + other * sine

    def project(w):
        return jnp.dot(x[...], w, preferred_element_type=jnp.float32).astype(jnp.bfloat16).astype(jnp.float32)

    peak[...] = jnp.full_like(peak, -1e30)
    acc[...] = jnp.zeros_like(acc)

    loads[0].wait()
    pl.semaphore_wait(
        barrier, jnp.minimum(below, REACH) + jnp.minimum(above, REACH) + members - 1 + n_tp - 1)
    x_copies = []
    for step in range(1, n_tp):
        mine = x.at[own_slice(tp)]
        copy = tp_copy(mine, mine, x_send.at[step], x_recv.at[step], (tp + step) % n_tp)
        copy.start()
        x_copies.append(copy)
    for step in range(1, n_tp):
        theirs = x.at[own_slice((tp + n_tp - step) % n_tp)]
        tp_copy(theirs, theirs, x_send.at[step], x_recv.at[step], (tp + step) % n_tp).wait_recv()

    for i in range(len(wkvs)):
        loads[1 + i].wait()
    if len(wkvs) == 2:
        keys = project(wkvs[0][...])
        vals = project(wkvs[1][...])
        for pair in range(members // 2):
            cut = slice(pair * LANES, (pair + 1) * LANES)
            k, v = turned(keys[:, cut], gain_k), vals[:, cut]
            kv_out[2 * pair] = jnp.where(even, k, pltpu.roll(v, head_dim, 1)).astype(jnp.bfloat16)
            kv_out[2 * pair + 1] = jnp.where(even, pltpu.roll(k, head_dim, 1), v).astype(jnp.bfloat16)
    else:
        both = project(wkvs[0][...])
        kv_out[0] = jnp.where(even, turned(both, gain_k), both).astype(jnp.bfloat16)

    kv_all[sp] = kv_out[member]

    def kv_copy(step):
        to = (member + step) % members
        return sp_copy(kv_out.at[to], kv_all.at[sp], kv_send.at[step], kv_recv.at[sp], first + to)

    for step in range(1, members):
        kv_copy(step).start()

    def line_copy(i, c):
        slot = kv_all.at[first + c]
        return sp_copy(slot, slot, line_send.at[i * members + c], kv_recv.at[first + c], nearest(i) * members + member)

    def onward(i, act):
        distance, side = way(i)

        @pl.when((distance >= REACH) & (plane - side >= 0) & (plane - side < groups))
        def _():
            for c in range(members):
                slot = (plane + distance * side) * members + c
                act(sp_copy(kv_all.at[slot], kv_all.at[slot], on_send.at[i * members + c], kv_recv.at[slot],
                            (plane - side) * members + member))

    def along(step):
        def one(i, carry):
            @pl.when(way(i)[0] <= REACH)
            def _():
                line_copy(i, (member + step) % members).start()
            return carry

        lax.fori_loop(1, groups, one, 0)

    along(0)

    def wait_kv(slot):
        sp_copy(kv_all.at[slot], kv_all.at[slot], kv_send.at[0], kv_recv.at[slot], sp).wait_recv()

    loads[1 + len(wkvs)].wait()
    for p in range(members):
        u = project(wq[:, p * width:(p + 1) * width])
        for t in range(width // LANES):
            cut = slice(t * LANES, (t + 1) * LANES)
            q_out[p, :, cut] = turned(u[:, cut], gain_q).astype(jnp.bfloat16)

    def q_copy(step):
        to = (member + step) % members
        return sp_copy(q_out.at[to], q_all.at[member], q_send.at[step], q_recv.at[member], first + to)

    for step in range(1, members):
        q_copy(step).start()
    q_all[member] = q_out[member]

    for step in range(1, members):
        wait_kv(first + (member + members - step) % members)
        along(members - step)

    wide_lane = lax.broadcasted_iota(jnp.int32, (rows, width), 1) // head_dim

    def mask_queries(c):
        q = q_all[c]
        for g in range(heads):
            qm[pl.ds(pl.multiple_of((c * heads + g) * rows, rows), rows), :] = jnp.where(
                wide_lane == g, q, jnp.zeros_like(q))

    tall = heads * rows

    def prepare(slot, c):
        tile = kv_all[slot].astype(jnp.float32)
        turned_tile = pltpu.roll(tile, head_dim, 1)
        kk = jnp.where(even, tile, turned_tile).astype(jnp.bfloat16)
        place = pl.ds(c * rows, rows)
        for t in range(width // LANES):
            k4[place, t * LANES:(t + 1) * LANES] = kk
        v1[place, :] = jnp.where(even, turned_tile, 1.0).astype(jnp.bfloat16)

    def attend(c):
        place = pl.ds(pl.multiple_of(c * tall, tall), tall)
        scores = lax.dot_general(qm[place, :], k4[...], (((1,), (1,)), ((), ())),
                                 preferred_element_type=jnp.float32)
        before = peak[place, :]
        now = jnp.maximum(before, jnp.max(scores, axis=1, keepdims=True))
        expo = jnp.exp(scores - jnp.concatenate([now] * (scores.shape[1] // LANES), axis=1))
        peak[place, :] = now
        acc[place, :] = acc[place, :] * jnp.exp(before - now) + jnp.dot(
            expo.astype(jnp.bfloat16), v1[...], preferred_element_type=jnp.float32)

    def finish(c):
        parts = []
        for pair in range(heads // 2):
            halves = []
            for g in (2 * pair, 2 * pair + 1):
                piece = acc[pl.ds(pl.multiple_of((c * heads + g) * rows, rows), rows), :]
                halves.append(piece / pltpu.roll(piece, head_dim, 1))
            parts.append(jnp.where(even, halves[0], pltpu.roll(halves[1], head_dim, 1)))
        m_out[c] = jnp.concatenate(parts, axis=1).astype(jnp.bfloat16)

    def m_copy(step):
        to = (member + step) % members
        return sp_copy(m_out.at[to], m_all.at[member], m_send.at[step], m_recv.at[member], first + to)

    for c in range(members):
        prepare(first + c, c)
    for step in range(members):
        c = (member + members - step) % members
        if step:
            sp_copy(q_out.at[c], q_all.at[c], q_send.at[step], q_recv.at[c], first + c).wait_recv()
        mask_queries(c)
        attend(c)

    def fetch(i):
        base = nearest(i) * members
        for c in range(members):
            wait_kv(base + c)
        onward(i, lambda copy: copy.start())
        for c in range(members):
            prepare(base + c, c)

    def whole_group(i, carry):
        fetch(i)
        for c in range(members):
            attend(c)
        return carry

    lax.fori_loop(1, groups - 1, whole_group, 0)
    fetch(groups - 1)
    for step in range(1, members + 1):
        c = (member + step) % members
        attend(c)
        finish(c)
        if step < members:
            m_copy(step).start()
    m_all[member] = m_out[member]

    loads[2 + len(wkvs)].wait()
    for step in range(members):
        s = (member + members - step) % members
        if step:
            sp_copy(m_out.at[s], m_all.at[s], m_send.at[step], m_recv.at[s], first + s).wait_recv()
        term = jnp.dot(m_all[s], wo[pl.ds(pl.multiple_of(s * width, width), width), :],
                       preferred_element_type=jnp.float32)
        if step == 0:
            o_acc[...] = term
        else:
            o_acc[...] += term
    o_copies = []
    for step in range(1, n_tp):
        to = (tp + step) % n_tp
        o_out[step] = o_acc[own_slice(to), :].astype(jnp.bfloat16)
        copy = tp_copy(o_out.at[step], o_in.at[step], o_send.at[step], o_recv.at[step], to)
        copy.start()
        o_copies.append(copy)
    result = o_acc[own_slice(tp), :].astype(jnp.bfloat16).astype(jnp.float32)
    for step in range(1, n_tp):
        o_copies[step - 1].wait_recv()
        result = result + o_in[step].astype(jnp.float32)
    out_ref[...] = result.astype(jnp.bfloat16)

    for copy in x_copies + o_copies:
        copy.wait_send()
    for step in range(1, members):
        kv_copy(step).wait_send()
        q_copy(step).wait_send()
        m_copy(step).wait_send()

    def sent_along(i, carry):
        @pl.when(way(i)[0] <= REACH)
        def _():
            for c in range(members):
                line_copy(i, c).wait_send()

        onward(i, lambda copy: copy.wait_send())
        return carry

    lax.fori_loop(1, groups, sent_along, 0)


def solution(mesh):
    n_sp, n_tp = mesh.shape["sp"], mesh.shape["tp"]

    def body(tokens_in, w_query, w_key, w_value, w_out, q_gain, k_gain):
        head_dim = q_gain.shape[0]
        own_rows, depth = tokens_in.shape
        rows = own_rows * n_tp
        query_cols, key_cols = w_query.shape[1], w_key.shape[1]
        members = key_cols // head_dim
        width = query_cols // members
        heads = width // head_dim
        if key_cols % LANES:
            wkv = (jnp.concatenate([w_key, w_value], axis=1),)
        else:
            wkv = (w_key, w_value)
        row_table, col_table = tables(rows * n_sp, head_dim)
        bf, f32 = jnp.bfloat16, jnp.float32
        hbm = pl.BlockSpec(memory_space=pltpu.HBM)
        vmem = pl.BlockSpec(memory_space=pltpu.VMEM)
        dma = pltpu.SemaphoreType.DMA
        call = pl.pallas_call(
            functools.partial(kernel, n_sp, n_tp, members, head_dim),
            out_shape=jax.ShapeDtypeStruct((own_rows, w_out.shape[1]), bf),
            in_specs=[hbm, hbm, (hbm,) * len(wkv), hbm, vmem, vmem, vmem, vmem],
            out_specs=vmem,
            scratch_shapes=[
                pltpu.VMEM((rows, depth), bf),
                pltpu.VMEM(w_query.shape, bf),
                tuple(pltpu.VMEM(w.shape, bf) for w in wkv),
                pltpu.VMEM(w_out.shape, bf),
                pltpu.VMEM((members, rows, LANES), bf),
                pltpu.VMEM((n_sp, rows, LANES), bf),
                pltpu.VMEM((members, rows, width), bf),
                pltpu.VMEM((members, rows, width), bf),
                pltpu.VMEM((members * heads * rows, width), bf),
                pltpu.VMEM((members * rows, width), bf),
                pltpu.VMEM((members * rows, LANES), bf),
                pltpu.VMEM((members * heads * rows, LANES), f32),
                pltpu.VMEM((members * heads * rows, LANES), f32),
                pltpu.VMEM((members, rows, width), bf),
                pltpu.VMEM((members, rows, width), bf),
                pltpu.VMEM((rows, w_out.shape[1]), f32),
                pltpu.VMEM((n_tp, own_rows, w_out.shape[1]), bf),
                pltpu.VMEM((n_tp, own_rows, w_out.shape[1]), bf),
                dma((6,)),
                dma((n_tp,)), dma((n_tp,)),
                dma((members,)), dma((n_sp,)), dma((n_sp,)), dma((n_sp,)),
                dma((members,)), dma((members,)),
                dma((members,)), dma((members,)),
                dma((n_tp,)), dma((n_tp,)),
            ],
            compiler_params=pltpu.CompilerParams(
                collective_id=0, has_side_effects=True, vmem_limit_bytes=56 * 1024 * 1024),
        )
        return call(tokens_in, w_query, wkv, w_out, jnp.asarray(row_table), jnp.asarray(col_table),
                    q_gain.reshape(1, head_dim), k_gain.reshape(1, head_dim))

    return jax.shard_map(
        body,
        mesh=mesh,
        in_specs=(
            P(("sp", "tp"), None),
            P(None, "tp"),
            P(None, "tp"),
            P(None, "tp"),
            P("tp", None),
            P(),
            P(),
        ),
        out_specs=P(("sp", "tp"), None),
        check_vma=False,
    )
```

```python
import functools

import jax
import jax.numpy as jnp
import numpy as np
from jax import lax
from jax.experimental import pallas as pl
from jax.experimental.pallas import tpu as pltpu
from jax.sharding import PartitionSpec as P

GRID_W = 64
LANES = 128
REACH = 1 << 20


def tables(token_count, head_dim):
    pairs = head_dim // 4
    lane = np.arange(LANES)
    freq = 10000.0 ** (-(lane % pairs) / pairs)
    sign = np.where(lane % (2 * pairs) < pairs, -1.0, 1.0)

    def both(count):
        angle = np.arange(count)[:, None] * freq[None, :]
        return np.concatenate([np.cos(angle), np.sin(angle) * sign], axis=1).astype(np.float32)

    return both(token_count // GRID_W), both(GRID_W)


def kernel(
    n_sp, n_tp, members, head_dim,
    tok_hbm, wq_hbm, wkv_hbms, wo_hbm, row_ref, col_ref, qg_ref, kg_ref, out_ref,
    x, wq, wkvs, wo, kv_out, kv_all, q_out, q_all, qm, k4, v1, peak, acc, m_out, m_all, o_acc, o_out, o_in,
    load_sem, x_send, x_recv, kv_send, kv_recv, line_send, on_send, q_send, q_recv, m_send, m_recv, o_send, o_recv,
):
    sp, tp = lax.axis_index("sp"), lax.axis_index("tp")
    own_rows = tok_hbm.shape[0]
    rows = own_rows * n_tp
    groups = n_sp // members
    plane, member = sp // members, sp % members
    query_cols = wq.shape[1]
    width = query_cols // members
    heads = width // head_dim
    first = plane * members

    def sp_copy(src, dst, send, recv, to):
        return pltpu.make_async_remote_copy(
            src_ref=src, dst_ref=dst, send_sem=send, recv_sem=recv,
            device_id={"sp": to}, device_id_type=pl.DeviceIdType.MESH)

    def tp_copy(src, dst, send, recv, to):
        return pltpu.make_async_remote_copy(
            src_ref=src, dst_ref=dst, send_sem=send, recv_sem=recv,
            device_id={"tp": to}, device_id_type=pl.DeviceIdType.MESH)

    def own_slice(index):
        return pl.ds(pl.multiple_of(index * own_rows, own_rows), own_rows)

    below, above = plane, groups - 1 - plane
    both_sides = jnp.minimum(below, above)

    def way(i):
        paired = i <= 2 * both_sides
        distance = jnp.where(paired, (i + 1) // 2, i - both_sides)
        upward = jnp.where(paired, i % 2, jnp.where(above > below, 1, 0))
        return distance, 2 * upward - 1

    def nearest(i):
        distance, side = way(i)
        return plane + distance * side

    loads = [pltpu.make_async_copy(tok_hbm, x.at[own_slice(tp)], load_sem.at[0])]
    for i, (src, dst) in enumerate(zip((*wkv_hbms, wq_hbm, wo_hbm), (*wkvs, wq, wo))):
        loads.append(pltpu.make_async_copy(src, dst, load_sem.at[i + 1]))
    for load in loads:
        load.start()
    barrier = pltpu.get_barrier_semaphore()
    for step in range(1, n_tp):
        pl.semaphore_signal(barrier, inc=1, device_id={"tp": (tp + step) % n_tp}, device_id_type=pl.DeviceIdType.MESH)

    for step in range(1, members):
        pl.semaphore_signal(barrier, inc=1, device_id={"sp": first + (member + step) % members},
                            device_id_type=pl.DeviceIdType.MESH)

    def greet(i, carry):
        @pl.when(way(i)[0] <= REACH)
        def _():
            pl.semaphore_signal(barrier, inc=1, device_id={"sp": nearest(i) * members + member},
                                device_id_type=pl.DeviceIdType.MESH)
        return carry

    lax.fori_loop(1, groups, greet, 0)

    lane = lax.broadcasted_iota(jnp.int32, (rows, LANES), 1)
    low = lane % head_dim < head_dim // 2
    left = lane % (head_dim // 2) < head_dim // 4
    even = lane < head_dim
    cos_parts, sin_parts = [], []
    per_dev = rows // GRID_W
    low_g = low[:GRID_W]
    for i in range(per_dev):
        line = row_ref[pl.ds(sp * per_dev + i, 1), :]
        cos_parts.append(jnp.where(low_g, jnp.broadcast_to(line[:, :LANES], (GRID_W, LANES)), col_ref[:, :LANES]))
        sin_parts.append(jnp.where(low_g, jnp.broadcast_to(line[:, LANES:], (GRID_W, LANES)), col_ref[:, LANES:]))
    cosine = jnp.concatenate(cos_parts, axis=0)
    sine = jnp.concatenate(sin_parts, axis=0)
    ones_r = lax.broadcasted_iota(jnp.int32, (LANES, LANES), 0) // head_dim
    ones_c = lax.broadcasted_iota(jnp.int32, (LANES, LANES), 1) // head_dim
    block = jnp.where(ones_r == ones_c, 1.0, 0.0).astype(jnp.bfloat16)
    gain_q = jnp.concatenate([qg_ref[...]] * (LANES // head_dim), axis=1) * head_dim ** (-0.5)
    gain_k = jnp.concatenate([kg_ref[...]] * (LANES // head_dim), axis=1)

    def turned(u, gain):
        square = u * u
        high = square.astype(jnp.bfloat16)
        rest = (square - high.astype(jnp.float32)).astype(jnp.bfloat16)
        total = jnp.dot(high, block, preferred_element_type=jnp.float32) + jnp.dot(
            rest, block, preferred_element_type=jnp.float32)
        n = u * lax.rsqrt(total * (1.0 / head_dim) + 1e-06) * gain
        quarter = head_dim // 4
        other = jnp.where(left, pltpu.roll(n, LANES - quarter, 1), pltpu.roll(n, quarter, 1))
        return n * cosine + other * sine

    def project(w):
        return jnp.dot(x[...], w, preferred_element_type=jnp.float32).astype(jnp.bfloat16).astype(jnp.float32)

    peak[...] = jnp.full_like(peak, -1e30)
    acc[...] = jnp.zeros_like(acc)

    loads[0].wait()
    pl.semaphore_wait(
        barrier, jnp.minimum(below, REACH) + jnp.minimum(above, REACH) + members - 1 + n_tp - 1)
    x_copies = []
    for step in range(1, n_tp):
        mine = x.at[own_slice(tp)]
        copy = tp_copy(mine, mine, x_send.at[step], x_recv.at[step], (tp + step) % n_tp)
        copy.start()
        x_copies.append(copy)
    for step in range(1, n_tp):
        theirs = x.at[own_slice((tp + n_tp - step) % n_tp)]
        tp_copy(theirs, theirs, x_send.at[step], x_recv.at[step], (tp + step) % n_tp).wait_recv()

    for i in range(len(wkvs)):
        loads[1 + i].wait()
    if len(wkvs) == 2:
        keys = project(wkvs[0][...])
        vals = project(wkvs[1][...])
        for pair in range(members // 2):
            cut = slice(pair * LANES, (pair + 1) * LANES)
            k, v = turned(keys[:, cut], gain_k), vals[:, cut]
            kv_out[2 * pair] = jnp.where(even, k, pltpu.roll(v, head_dim, 1)).astype(jnp.bfloat16)
            kv_out[2 * pair + 1] = jnp.where(even, pltpu.roll(k, head_dim, 1), v).astype(jnp.bfloat16)
    else:
        both = project(wkvs[0][...])
        kv_out[0] = jnp.where(even, turned(both, gain_k), both).astype(jnp.bfloat16)

    kv_all[sp] = kv_out[member]

    def kv_copy(step):
        to = (member + step) % members
        return sp_copy(kv_out.at[to], kv_all.at[sp], kv_send.at[step], kv_recv.at[sp], first + to)

    for step in range(1, members):
        kv_copy(step).start()

    def line_copy(i, c):
        slot = kv_all.at[first + c]
        return sp_copy(slot, slot, line_send.at[i * members + c], kv_recv.at[first + c], nearest(i) * members + member)

    def onward(i, act):
        distance, side = way(i)

        @pl.when((distance >= REACH) & (plane - side >= 0) & (plane - side < groups))
        def _():
            for c in range(members):
                slot = (plane + distance * side) * members + c
                act(sp_copy(kv_all.at[slot], kv_all.at[slot], on_send.at[i * members + c], kv_recv.at[slot],
                            (plane - side) * members + member))

    def along(step):
        def one(i, carry):
            @pl.when(way(i)[0] <= REACH)
            def _():
                line_copy(i, (member + step) % members).start()
            return carry

        lax.fori_loop(1, groups, one, 0)

    along(0)

    def wait_kv(slot):
        sp_copy(kv_all.at[slot], kv_all.at[slot], kv_send.at[0], kv_recv.at[slot], sp).wait_recv()

    loads[1 + len(wkvs)].wait()
    for p in range(members):
        u = project(wq[:, p * width:(p + 1) * width])
        for t in range(width // LANES):
            cut = slice(t * LANES, (t + 1) * LANES)
            q_out[p, :, cut] = turned(u[:, cut], gain_q).astype(jnp.bfloat16)

    def q_copy(step):
        to = (member + step) % members
        return sp_copy(q_out.at[to], q_all.at[member], q_send.at[step], q_recv.at[member], first + to)

    for step in range(1, members):
        q_copy(step).start()
    q_all[member] = q_out[member]

    for step in range(1, members):
        wait_kv(first + (member + members - step) % members)
        along(members - step)

    wide_lane = lax.broadcasted_iota(jnp.int32, (rows, width), 1) // head_dim

    def mask_queries(c):
        q = q_all[c]
        for g in range(heads):
            qm[pl.ds(pl.multiple_of((c * heads + g) * rows, rows), rows), :] = jnp.where(
                wide_lane == g, q, jnp.zeros_like(q))

    tall = heads * rows

    def prepare(slot, c):
        tile = kv_all[slot].astype(jnp.float32)
        turned_tile = pltpu.roll(tile, head_dim, 1)
        kk = jnp.where(even, tile, turned_tile).astype(jnp.bfloat16)
        place = pl.ds(c * rows, rows)
        for t in range(width // LANES):
            k4[place, t * LANES:(t + 1) * LANES] = kk
        v1[place, :] = jnp.where(even, turned_tile, 1.0).astype(jnp.bfloat16)

    def attend(c):
        place = pl.ds(pl.multiple_of(c * tall, tall), tall)
        scores = lax.dot_general(qm[place, :], k4[...], (((1,), (1,)), ((), ())),
                                 preferred_element_type=jnp.float32)
        before = peak[place, :]
        now = jnp.maximum(before, jnp.max(scores, axis=1, keepdims=True))
        expo = jnp.exp(scores - jnp.concatenate([now] * (scores.shape[1] // LANES), axis=1))
        peak[place, :] = now
        acc[place, :] = acc[place, :] * jnp.exp(before - now) + jnp.dot(
            expo.astype(jnp.bfloat16), v1[...], preferred_element_type=jnp.float32)

    def finish(c):
        parts = []
        for pair in range(heads // 2):
            halves = []
            for g in (2 * pair, 2 * pair + 1):
                piece = acc[pl.ds(pl.multiple_of((c * heads + g) * rows, rows), rows), :]
                halves.append(piece / pltpu.roll(piece, head_dim, 1))
            parts.append(jnp.where(even, halves[0], pltpu.roll(halves[1], head_dim, 1)))
        m_out[c] = jnp.concatenate(parts, axis=1).astype(jnp.bfloat16)

    def m_copy(step):
        to = (member + step) % members
        return sp_copy(m_out.at[to], m_all.at[member], m_send.at[step], m_recv.at[member], first + to)

    for c in range(members):
        prepare(first + c, c)
    for step in range(members):
        c = (member + members - step) % members
        if step:
            sp_copy(q_out.at[c], q_all.at[c], q_send.at[step], q_recv.at[c], first + c).wait_recv()
        mask_queries(c)
        attend(c)

    def fetch(i):
        base = nearest(i) * members
        for c in range(members):
            wait_kv(base + c)
        onward(i, lambda copy: copy.start())
        for c in range(members):
            prepare(base + c, c)

    def whole_group(i, carry):
        fetch(i)
        for c in range(members):
            attend(c)
        return carry

    lax.fori_loop(1, groups - 1, whole_group, 0)
    fetch(groups - 1)
    for step in range(1, members + 1):
        c = (member + step) % members
        attend(c)
        finish(c)
        if step < members:
            m_copy(step).start()
    m_all[member] = m_out[member]

    loads[2 + len(wkvs)].wait()
    for step in range(members):
        s = (member + members - step) % members
        if step:
            sp_copy(m_out.at[s], m_all.at[s], m_send.at[step], m_recv.at[s], first + s).wait_recv()
        term = jnp.dot(m_all[s], wo[pl.ds(pl.multiple_of(s * width, width), width), :],
                       preferred_element_type=jnp.float32)
        if step == 0:
            o_acc[...] = term
        else:
            o_acc[...] += term
    o_copies = []
    for step in range(1, n_tp):
        to = (tp + step) % n_tp
        o_out[step] = o_acc[own_slice(to), :].astype(jnp.bfloat16)
        copy = tp_copy(o_out.at[step], o_in.at[step], o_send.at[step], o_recv.at[step], to)
        copy.start()
        o_copies.append(copy)
    result = o_acc[own_slice(tp), :].astype(jnp.bfloat16).astype(jnp.float32)
    for step in range(1, n_tp):
        o_copies[step - 1].wait_recv()
        result = result + o_in[step].astype(jnp.float32)
    out_ref[...] = result.astype(jnp.bfloat16)

    for copy in x_copies + o_copies:
        copy.wait_send()
    for step in range(1, members):
        kv_copy(step).wait_send()
        q_copy(step).wait_send()
        m_copy(step).wait_send()

    def sent_along(i, carry):
        @pl.when(way(i)[0] <= REACH)
        def _():
            for c in range(members):
                line_copy(i, c).wait_send()

        onward(i, lambda copy: copy.wait_send())
        return carry

    lax.fori_loop(1, groups, sent_along, 0)


def solution(mesh):
    n_sp, n_tp = mesh.shape["sp"], mesh.shape["tp"]

    def body(tokens_in, w_query, w_key, w_value, w_out, q_gain, k_gain):
        head_dim = q_gain.shape[0]
        own_rows, depth = tokens_in.shape
        rows = own_rows * n_tp
        query_cols, key_cols = w_query.shape[1], w_key.shape[1]
        members = key_cols // head_dim
        width = query_cols // members
        heads = width // head_dim
        if key_cols % LANES:
            wkv = (jnp.concatenate([w_key, w_value], axis=1),)
        else:
            wkv = (w_key, w_value)
        row_table, col_table = tables(rows * n_sp, head_dim)
        bf, f32 = jnp.bfloat16, jnp.float32
        hbm = pl.BlockSpec(memory_space=pltpu.HBM)
        vmem = pl.BlockSpec(memory_space=pltpu.VMEM)
        dma = pltpu.SemaphoreType.DMA
        call = pl.pallas_call(
            functools.partial(kernel, n_sp, n_tp, members, head_dim),
            out_shape=jax.ShapeDtypeStruct((own_rows, w_out.shape[1]), bf),
            in_specs=[hbm, hbm, (hbm,) * len(wkv), hbm, vmem, vmem, vmem, vmem],
            out_specs=vmem,
            scratch_shapes=[
                pltpu.VMEM((rows, depth), bf),
                pltpu.VMEM(w_query.shape, bf),
                tuple(pltpu.VMEM(w.shape, bf) for w in wkv),
                pltpu.VMEM(w_out.shape, bf),
                pltpu.VMEM((members, rows, LANES), bf),
                pltpu.VMEM((n_sp, rows, LANES), bf),
                pltpu.VMEM((members, rows, width), bf),
                pltpu.VMEM((members, rows, width), bf),
                pltpu.VMEM((members * heads * rows, width), bf),
                pltpu.VMEM((members * rows, width), bf),
                pltpu.VMEM((members * rows, LANES), bf),
                pltpu.VMEM((members * heads * rows, LANES), f32),
                pltpu.VMEM((members * heads * rows, LANES), f32),
                pltpu.VMEM((members, rows, width), bf),
                pltpu.VMEM((members, rows, width), bf),
                pltpu.VMEM((rows, w_out.shape[1]), f32),
                pltpu.VMEM((n_tp, own_rows, w_out.shape[1]), bf),
                pltpu.VMEM((n_tp, own_rows, w_out.shape[1]), bf),
                dma((6,)),
                dma((n_tp,)), dma((n_tp,)),
                dma((members,)), dma((n_sp,)), dma((n_sp,)), dma((n_sp,)),
                dma((members,)), dma((members,)),
                dma((members,)), dma((members,)),
                dma((n_tp,)), dma((n_tp,)),
            ],
            compiler_params=pltpu.CompilerParams(
                collective_id=0, has_side_effects=True, vmem_limit_bytes=56 * 1024 * 1024),
        )
        return call(tokens_in, w_query, wkv, w_out, jnp.asarray(row_table), jnp.asarray(col_table),
                    q_gain.reshape(1, head_dim), k_gain.reshape(1, head_dim))

    return jax.shard_map(
        body,
        mesh=mesh,
        in_specs=(
            P(("sp", "tp"), None),
            P(None, "tp"),
            P(None, "tp"),
            P(None, "tp"),
            P("tp", None),
            P(),
            P(),
        ),
        out_specs=P(("sp", "tp"), None),
        check_vma=False,
    )
```
